32 devices in a mesh: fs: 16 (over z, y, x), tp: 2 (over core).
Axes of the slice: x: 2, y: 2, z: 4, core: 2. Of those that a mesh axis runs over, the one named last changes fastest.
Arguments:
- normed: bfloat16 [16384, 2048], P('fs'), may hold values from -6 to 6
- key_cot: bfloat16 [16384, 1024], P('fs', 'tp'), may hold values from -130 to 130
- value_cot: bfloat16 [16384, 2048], P('fs', 'tp'), may hold values from -130 to 130
- basis: bfloat16 [2048, 256], P('fs'), may hold values from -3.535534 to 3.535534
- master_key: float32 [2048, 1024], P('fs', 'tp'), may hold values from -3 to 3
- master_value: float32 [2048, 2048], P('fs', 'tp'), may hold values from -3 to 3
- first_key: float32 [256, 1024], P('fs', 'tp'), may hold values from -3 to 3
- second_key: float32 [256, 1024], P('fs', 'tp'), may hold values from 0.05 to 2
- first_value: float32 [256, 2048], P('fs', 'tp'), may hold values from -3 to 3
- second_value: float32 [256, 2048], P('fs', 'tp'), may hold values from 0.05 to 2
Outputs:
- step_key: float32 [2048, 1024], P('fs', 'tp')
- step_value: float32 [2048, 2048], P('fs', 'tp')
- new_master_key: float32 [2048, 1024], P('fs', 'tp')
- new_master_value: float32 [2048, 2048], P('fs', 'tp')
- copy_key: bfloat16 [2048, 1024], P(None, 'tp')
- copy_value: bfloat16 [2048, 2048], P(None, 'tp')
- new_first_key: float32 [256, 1024], P('fs', 'tp')
- new_second_key: float32 [256, 1024], P('fs', 'tp')
- new_first_value: float32 [256, 2048], P('fs', 'tp')
- new_second_value: float32 [256, 2048], P('fs', 'tp')
The draws below stay inside these ranges and needn't reach their ends.
All inputs are finite; a program needn't handle non-finite values.
Results may differ from the reference program's by a relative error of at most 0.0055.
Values may be sent and summed in bfloat16 or wider, within the bound.
A program may use at most 64 MiB of HBM per device.

```python
import math
import jax
import jax.numpy as jnp
from jax import lax

D = 2048
DK = 1024
DV = 2048
R = 256
TOKENS = 16384


def column_scaled(key, height, width):
    keys = jax.random.split(key, 2)
    ramp = jnp.arange(width, dtype=jnp.float32) / max(width - 1, 1)
    jitter = jnp.exp(jax.random.uniform(keys[1], (width,), jnp.float32, math.log(0.7), math.log(1.4)))
    scales = 10.0 ** ramp * jitter
    base_values = jnp.clip(jax.random.normal(keys[0], (height, width), jnp.float32), -6.0, 6.0)
    return base_values * scales[None, :]


def draw_basis(key, part):
    values = column_scaled(jax.random.fold_in(key, 11), D, R) * D ** (-0.5)
    return values.astype(jnp.bfloat16)


def draw_key_cot(key, part):
    return column_scaled(jax.random.fold_in(key, 12), TOKENS, DK).astype(jnp.bfloat16)


def draw_value_cot(key, part):
    return column_scaled(jax.random.fold_in(key, 13), TOKENS, DV).astype(jnp.bfloat16)


def shard_levels(stream_key, dims, cuts, low, largest):
    factor_of, own = 1.0, jax.random.fold_in(stream_key, 6)
    for dim, blocks in cuts:
        steps = jnp.exp(jax.random.uniform(jax.random.fold_in(own, dim), (blocks,), jnp.float32, low / len(cuts), largest / len(cuts)))
        factor_of = factor_of * jnp.repeat(steps, dims[dim] // blocks).reshape([-1 if axis == dim else 1 for axis in range(len(dims))])
    return factor_of


def noise(stream_key, extent, deviation, limit, cuts=(), kind=jnp.bfloat16):
    gain = shard_levels(stream_key, extent, cuts, -0.22, 0.18) if cuts else 1.0
    drawn = jax.random.normal(stream_key, extent, jnp.float32) * deviation * gain
    return jnp.minimum(jnp.maximum(drawn, -limit), limit).astype(kind)


def setup_inputs(seed: int = 0) -> dict:
    arg_keys = jax.random.split(jax.random.key(seed), 11)
    return {
        "normed": noise(arg_keys[0], (TOKENS, D), 1.0, 6.0, ((0, 16),)),
        "key_cot": draw_key_cot(jax.random.fold_in(arg_keys[10], 71), 0),
        "value_cot": draw_value_cot(jax.random.fold_in(arg_keys[10], 71), 0),
        "basis": draw_basis(jax.random.fold_in(arg_keys[10], 71), 0),
        "master_key": noise(arg_keys[4], (D, DK), 0.5, 3.0, ((0, 16), (1, 2)), jnp.float32),
        "master_value": noise(arg_keys[5], (D, DV), 0.5, 3.0, ((0, 16), (1, 2)), jnp.float32),
        "first_key": noise(arg_keys[6], (R, DK), 0.5, 3.0, ((0, 16), (1, 2)), jnp.float32),
        "second_key": jnp.clip(jnp.exp(math.log(2.0) - 3.6888794 * jax.random.uniform(arg_keys[7], (R, DK), jnp.float32) ** shard_levels(arg_keys[7], (R, DK), ((0, 16), (1, 2)), -0.2, 0.2)), 0.05, 2.0),
        "first_value": noise(arg_keys[8], (R, DV), 0.5, 3.0, ((0, 16), (1, 2)), jnp.float32),
        "second_value": jnp.clip(jnp.exp(math.log(2.0) - 3.6888794 * jax.random.uniform(arg_keys[9], (R, DV), jnp.float32) ** shard_levels(arg_keys[9], (R, DV), ((0, 16), (1, 2)), -0.2, 0.2)), 0.05, 2.0),
    }


learn_rate = 0.05
beta_first = 0.9
beta_second = 0.9
epsilon = 1e-08
norm_eps = 1e-06

def moment_update(low_grad, grad_scale, first_moment, second_moment, basis):
    scaled = low_grad * grad_scale
    new_first = beta_first * first_moment + (1.0 - beta_first) * scaled
    new_second = beta_second * second_moment + (1.0 - beta_second) * scaled * scaled
    direction = (new_first / (jnp.sqrt(new_second) + epsilon)).astype(jnp.bfloat16)
    update_step = jnp.dot(basis, direction, preferred_element_type=jnp.float32)
    return (update_step, new_first, new_second)

def reference(normed, key_cot, value_cot, basis, master_key, master_value, first_key, second_key, first_value, second_value):
    grad_key = jnp.dot(normed.T, key_cot, preferred_element_type=jnp.float32)
    grad_value = jnp.dot(normed.T, value_cot, preferred_element_type=jnp.float32)
    basis_wide = basis.astype(jnp.float32).T
    low_key = jnp.dot(basis_wide, grad_key, precision=lax.Precision.HIGHEST, preferred_element_type=jnp.float32)
    low_value = jnp.dot(basis_wide, grad_value, precision=lax.Precision.HIGHEST, preferred_element_type=jnp.float32)
    squares = jnp.sum(low_key * low_key) + jnp.sum(low_value * low_value)
    root_mean = jnp.sqrt(squares / (R * (DK + DV)) + norm_eps)
    grad_scale = 1.0 / root_mean
    step_key, new_first_key, new_second_key = moment_update(low_key, grad_scale, first_key, second_key, basis)
    step_value, new_first_value, new_second_value = moment_update(low_value, grad_scale, first_value, second_value, basis)
    new_master_key = master_key - learn_rate * step_key
    new_master_value = master_value - learn_rate * step_value
    return (step_key, step_value, new_master_key, new_master_value, new_master_key.astype(jnp.bfloat16), new_master_value.astype(jnp.bfloat16), new_first_key, new_second_key, new_first_value, new_second_value)
```

```python
import functools

import jax
import jax.numpy as jnp
from jax import lax
from jax.experimental import pallas as pl
from jax.experimental.pallas import tpu as pltpu
from jax.sharding import PartitionSpec as P

learn_rate = 0.05
beta_first = 0.9
beta_second = 0.9
epsilon = 1e-08
norm_eps = 1e-06

MESH = pl.DeviceIdType.MESH
F32 = jnp.float32
BF16 = jnp.bfloat16


class Gather:
    def __init__(self, lines, slot, own, send_sem, recv_sem):
        self.lines, self.slot, self.own = lines, slot, own
        self.send_sem, self.recv_sem = send_sem, recv_sem
        self.me = lax.axis_index("fs")
        self.z = self.me // 4
        self.y = lax.rem(self.me // 2, 2)
        self.x = lax.rem(self.me, 2)
        self.sent = []

    def at(self, i, fy, fx):
        y = 1 - self.y if fy else self.y
        x = 1 - self.x if fx else self.x
        return lax.rem(self.z - i + self.lines, self.lines) * 4 + y * 2 + x

    def send(self, part, index, source, owner, target):
        copy = pltpu.make_async_remote_copy(
            src_ref=source,
            dst_ref=self.slot(owner, part),
            send_sem=self.send_sem.at[part, index],
            recv_sem=self.recv_sem.at[part, index],
            device_id={"fs": target},
            device_id_type=MESH,
        )
        copy.start()
        self.sent.append(copy)

    def arrive(self, part, index, owner):
        place = self.slot(owner, part)
        pltpu.make_async_remote_copy(
            src_ref=place,
            dst_ref=place,
            send_sem=self.send_sem.at[part, index],
            recv_sem=self.recv_sem.at[part, index],
            device_id={"fs": self.at(0, 0, 1)},
            device_id_type=MESH,
        ).wait_recv()

    def flips(self, part):
        return ((1, 0), (0, 1)) if part == 0 else ((0, 1), (1, 0))

    def along_z(self):
        for part in range(2):
            for k in range(1, self.lines):
                self.send(part, k, self.own(part), self.me, self.at(self.lines - k, 0, 0))

    def hop_one(self, part, i):
        first, _ = self.flips(part)
        owner = self.at(i, 0, 0)
        source = self.own(part) if i == 0 else self.slot(owner, part)
        self.send(part, self.lines + i, source, owner, self.at(0, *first))

    def hop_two(self, part, i, flipped):
        first, second = self.flips(part)
        owner = self.at(i, *first) if flipped else self.at(i, 0, 0)
        source = self.own(part) if i == 0 and not flipped else self.slot(owner, part)
        self.send(part, (3 if flipped else 2) * self.lines + i, source, owner, self.at(0, *second))

    def steps(self):
        def begin():
            for part in range(2):
                self.hop_one(part, 0)
            for part in range(2):
                self.hop_two(part, 0, False)

        def from_line(i):
            for part in range(2):
                self.arrive(part, i, self.at(i, 0, 0))
                self.hop_one(part, i)
            for part in range(2):
                self.hop_two(part, i, False)

        def from_first(i):
            for part in range(2):
                first, _ = self.flips(part)
                self.arrive(part, self.lines + i, self.at(i, *first))
                self.hop_two(part, i, True)

        def from_second(i):
            for part in range(2):
                first, second = self.flips(part)
                self.arrive(part, 2 * self.lines + i, self.at(i, *second))
                self.arrive(part, 3 * self.lines + i, self.at(i, 1, 1))

        out = [begin]
        for i in range(1, self.lines):
            out.append(functools.partial(from_line, i))
            out.append(functools.partial(from_first, i - 1))
        out.append(functools.partial(from_first, self.lines - 1))
        tail = [functools.partial(from_second, i) for i in range(self.lines)]
        return out, tail

    def close(self):
        for copy in self.sent:
            copy.wait_send()


def exchange_kernel(
    n,
    tp,
    count,
    normed,
    key_cot,
    value_cot,
    basis,
    master,
    first_key,
    second_key,
    first_value,
    second_value,
    basis_all,
    master_all,
    dirs_all,
    new_first_key,
    new_second_key,
    new_first_value,
    new_second_value,
    normed_v,
    key_v,
    value_v,
    projected,
    partial,
    received,
    direction,
    own_square,
    squares,
    chip_square,
    chip_squares,
    load_sem,
    basis_send,
    basis_recv,
    master_send,
    master_recv,
    dirs_send,
    dirs_recv,
    part_send,
    part_recv,
    square_send,
    square_recv,
    chip_send,
    chip_recv,
):
    me = lax.axis_index("fs")
    my_tp = lax.axis_index("tp")
    loads = [
        pltpu.make_async_copy(source, target, load_sem.at[i])
        for i, (source, target) in enumerate(((normed, normed_v), (key_cot, key_v), (value_cot, value_v)))
    ]
    for load in loads:
        load.start()

    barrier = pltpu.get_barrier_semaphore()
    for k in range(1, n):
        pl.semaphore_signal(barrier, inc=1, device_id={"fs": lax.rem(me + k, n)}, device_id_type=MESH)
    for k in range(1, tp):
        pl.semaphore_signal(barrier, inc=1, device_id={"tp": lax.rem(my_tp + k, tp)}, device_id_type=MESH)
    pl.semaphore_wait(barrier, n - 1 + tp - 1)

    lines = n // 4

    def gather(whole, own, send_sem, recv_sem, stacked):
        cols = own.shape[-1]
        cut = cols // 256 * 128
        spans = (pl.ds(0, cut), pl.ds(cut, cols - cut))
        rows = own.shape[0]

        def slot(owner, part):
            if stacked:
                return whole.at[owner, :, spans[part]]
            return whole.at[pl.ds(pl.multiple_of(owner * rows, rows), rows), spans[part]]

        return Gather(lines, slot, lambda part: own.at[:, spans[part]], send_sem, recv_sem)

    basis_g = gather(basis_all, basis, basis_send, basis_recv, False)
    master_g = gather(master_all, master, master_send, master_recv, False)
    dirs_g = gather(dirs_all, direction, dirs_send, dirs_recv, True)

    basis_g.along_z()
    steps, tail = basis_g.steps()
    steps[0]()
    master_g.along_z()
    rows = basis.shape[0]
    own_rows = pl.ds(pl.multiple_of(me * rows, rows), rows)
    basis_all[own_rows, :] = basis[...]
    master_all[own_rows, :] = master[...]
    for step in steps[1:]:
        step()
    master_steps, master_tail = master_g.steps()
    master_steps[0]()
    for step in tail:
        step()

    loads[0].wait()
    tokens = normed_v.shape[0]
    tile = 256

    @pl.loop(0, tokens // tile)
    def _(t):
        at = pl.ds(pl.multiple_of(t * tile, tile), tile)
        projected[at, :] = jnp.dot(normed_v[at, :], basis_all[...], preferred_element_type=F32).astype(BF16)

    loads[1].wait()
    loads[2].wait()
    kc = key_v.shape[1]
    rank_rows = first_key.shape[0]

    def project(cot, base):
        width = cot.shape[1]
        step = min(width, 512)
        for c in range(0, width, step):
            sums = lax.dot_general(
                projected[...], cot[:, c : c + step], (((0,), (0,)), ((), ())), preferred_element_type=F32
            ).astype(BF16)
            for j in range(n):
                partial[j, :, base + c : base + c + step] = sums[j * rank_rows : (j + 1) * rank_rows, :]

    project(key_v, 0)
    project(value_v, kc)

    part_copies = []
    for k in range(1, n):
        target = lax.rem(me + k, n)
        copy = pltpu.make_async_remote_copy(
            src_ref=partial.at[target],
            dst_ref=received.at[k],
            send_sem=part_send.at[k],
            recv_sem=part_recv.at[k],
            device_id={"fs": target},
            device_id_type=MESH,
        )
        copy.start()
        part_copies.append(copy)
    low = partial[me].astype(F32)
    received[0] = partial[me]
    for step in master_steps[1:]:
        step()
    for k, copy in enumerate(part_copies):
        copy.wait_recv()
    low = received[0].astype(F32)
    for k in range(1, n):
        low = low + received[k].astype(F32)

    square = jnp.sum(low * low)
    own_square[...] = jnp.full(own_square.shape, square, F32)
    squares[0] = jnp.full(own_square.shape, square, F32)
    square_copies = []
    for k in range(1, n):
        copy = pltpu.make_async_remote_copy(
            src_ref=own_square,
            dst_ref=squares.at[k],
            send_sem=square_send.at[k],
            recv_sem=square_recv.at[k],
            device_id={"fs": lax.rem(me + k, n)},
            device_id_type=MESH,
        )
        copy.start()
        square_copies.append(copy)
    for copy in square_copies:
        copy.wait_recv()
    chip_square[...] = jnp.sum(squares[...], axis=0)
    chip_squares[0] = jnp.sum(squares[...], axis=0)
    chip_copies = []
    for k in range(1, tp):
        copy = pltpu.make_async_remote_copy(
            src_ref=chip_square,
            dst_ref=chip_squares.at[k],
            send_sem=chip_send.at[k],
            recv_sem=chip_recv.at[k],
            device_id={"tp": lax.rem(my_tp + k, tp)},
            device_id_type=MESH,
        )
        copy.start()
        chip_copies.append(copy)
    for copy in chip_copies:
        copy.wait_recv()
    total = jnp.sum(chip_squares[...], axis=0)[0:1, 0:1]
    grad_scale = 1.0 / jnp.sqrt(total / count + norm_eps)

    def update(scaled, first, second, new_first, new_second, base):
        moved = beta_first * first[...] + (1.0 - beta_first) * scaled
        spread = beta_second * second[...] + (1.0 - beta_second) * scaled * scaled
        new_first[...] = moved
        new_second[...] = spread
        turned = (moved / (jnp.sqrt(spread) + epsilon)).astype(BF16)
        direction[:, base : base + turned.shape[1]] = turned
        dirs_all[me, :, base : base + turned.shape[1]] = turned

    scaled = low * grad_scale
    update(scaled[:, :kc], first_key, second_key, new_first_key, new_second_key, 0)
    update(scaled[:, kc:], first_value, second_value, new_first_value, new_second_value, kc)

    dirs_g.along_z()
    dirs_steps, dirs_tail = dirs_g.steps()
    for step in dirs_steps + dirs_tail + master_tail:
        step()
    for g in (basis_g, master_g, dirs_g):
        g.close()
    for copy in part_copies + square_copies + chip_copies:
        copy.wait_send()


def final_kernel(basis_all, master_all, dirs, basis, master_key, master_value, copy_key, copy_value, step_key, step_value, new_key, new_value):
    kc = copy_key.shape[1]
    for cut, out in ((slice(0, kc), copy_key), (slice(kc, None), copy_value)):
        step = jnp.dot(basis_all[...], dirs[:, cut], preferred_element_type=F32)
        out[...] = (master_all[:, cut].astype(F32) - learn_rate * step).astype(BF16)

    @pl.when(pl.program_id(0) == 0)
    def _():
        for cut, master, step_out, new in (
            (slice(0, kc), master_key, step_key, new_key),
            (slice(kc, None), master_value, step_value, new_value),
        ):
            step = jnp.dot(basis[...], dirs[:, cut], preferred_element_type=F32)
            step_out[...] = step
            new[...] = master[...] - learn_rate * step


def on_device(
    n,
    tp,
    normed,
    key_cot,
    value_cot,
    basis,
    master_key,
    master_value,
    first_key,
    second_key,
    first_value,
    second_value,
):
    rows, rank = basis.shape
    d = rows * n
    kc, vc = key_cot.shape[1], value_cot.shape[1]
    cols = kc + vc
    tokens = normed.shape[0]
    rank_rows = first_key.shape[0]
    lines = n // 4
    master = jnp.concatenate([master_key.astype(BF16), master_value.astype(BF16)], axis=1)
    vmem = pl.BlockSpec(memory_space=pltpu.VMEM)
    hbm = pl.BlockSpec(memory_space=pl.ANY)
    dma = pltpu.SemaphoreType.DMA
    small = (8, 128)
    basis_all, master_all, dirs, nfk, nsk, nfv, nsv = pl.pallas_call(
        functools.partial(exchange_kernel, n, tp, rank * cols * tp),
        out_shape=(
            jax.ShapeDtypeStruct((d, rank), BF16),
            jax.ShapeDtypeStruct((d, cols), BF16),
            jax.ShapeDtypeStruct((n, rank_rows, cols), BF16),
            jax.ShapeDtypeStruct(first_key.shape, F32),
            jax.ShapeDtypeStruct(first_key.shape, F32),
            jax.ShapeDtypeStruct(first_value.shape, F32),
            jax.ShapeDtypeStruct(first_value.shape, F32),
        ),
        in_specs=[hbm] * 3 + [vmem] * 6,
        out_specs=[vmem] * 7,
        scratch_shapes=[
            pltpu.VMEM(normed.shape, BF16),
            pltpu.VMEM(key_cot.shape, BF16),
            pltpu.VMEM(value_cot.shape, BF16),
            pltpu.VMEM((tokens, rank), BF16),
            pltpu.VMEM((n, rank_rows, cols), BF16),
            pltpu.VMEM((n, rank_rows, cols), BF16),
            pltpu.VMEM((rank_rows, cols), BF16),
            pltpu.VMEM(small, F32),
            pltpu.VMEM((n, *small), F32),
            pltpu.VMEM(small, F32),
            pltpu.VMEM((tp, *small), F32),
            dma((3,)),
        ]
        + [dma((2, 4 * lines))] * 6
        + [dma((n,))] * 4
        + [dma((tp,))] * 2,
        compiler_params=pltpu.CompilerParams(
            collective_id=0, has_side_effects=True, vmem_limit_bytes=50 * 1024 * 1024
        ),
    )(normed, key_cot, value_cot, basis, master, first_key, second_key, first_value, second_value)
    dirs = dirs.reshape(rank, cols)

    block = 256
    whole = lambda *shape: pl.BlockSpec(shape, lambda i: (0,) * len(shape))
    sliced = lambda width: pl.BlockSpec((block, width), lambda i: (i, 0))
    copy_key, copy_value, step_key, step_value, new_key, new_value = pl.pallas_call(
        final_kernel,
        grid=(d // block,),
        out_shape=(
            jax.ShapeDtypeStruct((d, kc), BF16),
            jax.ShapeDtypeStruct((d, vc), BF16),
            jax.ShapeDtypeStruct((rows, kc), F32),
            jax.ShapeDtypeStruct((rows, vc), F32),
            jax.ShapeDtypeStruct((rows, kc), F32),
            jax.ShapeDtypeStruct((rows, vc), F32),
        ),
        in_specs=[
            sliced(rank),
            sliced(cols),
            whole(rank, cols),
            whole(rows, rank),
            whole(rows, kc),
            whole(rows, vc),
        ],
        out_specs=[sliced(kc), sliced(vc), whole(rows, kc), whole(rows, vc), whole(rows, kc), whole(rows, vc)],
    )(basis_all, master_all, dirs, basis, master_key, master_value)
    return (step_key, step_value, new_key, new_value, copy_key, copy_value, nfk, nsk, nfv, nsv)


def solution(mesh):
    split = P("fs", "tp")
    lone = P("fs", None)
    return jax.shard_map(
        functools.partial(on_device, mesh.shape["fs"], mesh.shape["tp"]),
        mesh=mesh,
        in_specs=(lone, split, split, lone) + (split,) * 6,
        out_specs=(split,) * 4 + (P(None, "tp"),) * 2 + (split,) * 4,
        check_vma=False,
    )
```

```python
import functools

import jax
import jax.numpy as jnp
from jax import lax
from jax.experimental import pallas as pl
from jax.experimental.pallas import tpu as pltpu
from jax.sharding import PartitionSpec as P

learn_rate = 0.05
beta_first = 0.9
beta_second = 0.9
epsilon = 1e-08
norm_eps = 1e-06

SHARES = (16, 16, 16)

MESH = pl.DeviceIdType.MESH
F32 = jnp.float32
BF16 = jnp.bfloat16


class Gather:
    def __init__(self, lines, slot, own, send_sem, recv_sem):
        self.lines, self.slot, self.own = lines, slot, own
        self.send_sem, self.recv_sem = send_sem, recv_sem
        self.me = lax.axis_index("fs")
        self.z = self.me // 4
        self.y = lax.rem(self.me // 2, 2)
        self.x = lax.rem(self.me, 2)
        self.along = [self.partner(i) for i in range(lines)]
        self.sent = []

    def partner(self, i):
        out, bit = self.z, 1
        while bit <= i:
            if i & bit:
                out = out + bit - 2 * bit * lax.rem(self.z // bit, 2)
            bit *= 2
        return out

    def at(self, i, fy, fx):
        y = 1 - self.y if fy else self.y
        x = 1 - self.x if fx else self.x
        return self.along[i] * 4 + y * 2 + x

    def send(self, part, index, source, owner, target):
        copy = pltpu.make_async_remote_copy(
            src_ref=source,
            dst_ref=self.slot(owner, part),
            send_sem=self.send_sem.at[part, index],
            recv_sem=self.recv_sem.at[part, index],
            device_id={"fs": target},
            device_id_type=MESH,
        )
        copy.start()
        self.sent.append(copy)

    def arrive(self, part, index, owner):
        place = self.slot(owner, part)
        pltpu.make_async_remote_copy(
            src_ref=place,
            dst_ref=place,
            send_sem=self.send_sem.at[part, index],
            recv_sem=self.recv_sem.at[part, index],
            device_id={"fs": self.at(0, 0, 1)},
            device_id_type=MESH,
        ).wait_recv()

    def flips(self, part):
        return ((1, 0), (0, 1)) if part == 0 else ((0, 1), (1, 0))

    def along_z(self, start=1, stop=None):
        for k in range(start, stop or self.lines):
            for part in range(2):
                self.send(part, k, self.own(part), self.me, self.at(k, 0, 0))

    def hop_one(self, part, i):
        first, _ = self.flips(part)
        owner = self.at(i, 0, 0)
        source = self.own(part) if i == 0 else self.slot(owner, part)
        self.send(part, self.lines + i, source, owner, self.at(0, *first))

    def hop_two(self, part, i, flipped):
        first, second = self.flips(part)
        owner = self.at(i, *first) if flipped else self.at(i, 0, 0)
        source = self.own(part) if i == 0 and not flipped else self.slot(owner, part)
        self.send(part, (3 if flipped else 2) * self.lines + i, source, owner, self.at(0, *second))

    def steps(self):
        def begin():
            for part in range(2):
                self.hop_one(part, 0)
            for part in range(2):
                self.hop_two(part, 0, False)

        def from_line(i):
            for part in range(2):
                self.arrive(part, i, self.at(i, 0, 0))
                self.hop_one(part, i)
            for part in range(2):
                self.hop_two(part, i, False)

        def from_first(i):
            for part in range(2):
                first, _ = self.flips(part)
                self.arrive(part, self.lines + i, self.at(i, *first))
                self.hop_two(part, i, True)

        def from_second(i):
            for part in range(2):
                first, second = self.flips(part)
                self.arrive(part, 2 * self.lines + i, self.at(i, *second))
                self.arrive(part, 3 * self.lines + i, self.at(i, 1, 1))

        out = [begin]
        for i in range(1, self.lines):
            out.append(functools.partial(from_line, i))
            out.append(functools.partial(from_first, i - 1))
        out.append(functools.partial(from_first, self.lines - 1))
        tail = [functools.partial(from_second, i) for i in range(self.lines)]
        return out, tail

    def close(self):
        for copy in self.sent:
            copy.wait_send()


def exchange_kernel(
    n,
    tp,
    count,
    normed,
    key_cot,
    value_cot,
    basis_in,
    master_key,
    master_value,
    first_key_in,
    second_key_in,
    first_value_in,
    second_value_in,
    basis_all,
    master_all,
    dirs_all,
    scaled_out,
    normed_v,
    key_v,
    value_v,
    basis,
    master_key_v,
    master_value_v,
    first_key,
    second_key,
    first_value,
    second_value,
    master,
    projected,
    partial,
    received,
    direction,
    own_square,
    squares,
    chip_square,
    chip_squares,
    load_sem,
    basis_send,
    basis_recv,
    master_send,
    master_recv,
    dirs_send,
    dirs_recv,
    part_send,
    part_recv,
    square_send,
    square_recv,
    chip_send,
    chip_recv,
):
    me = lax.axis_index("fs")
    my_tp = lax.axis_index("tp")
    loads = [
        pltpu.make_async_copy(source, target, load_sem.at[i])
        for i, (source, target) in enumerate(
            (
                (basis_in, basis),
                (master_key, master_key_v),
                (master_value, master_value_v),
                (normed, normed_v),
                (key_cot, key_v),
                (value_cot, value_v),
                (first_key_in, first_key),
                (second_key_in, second_key),
                (first_value_in, first_value),
                (second_value_in, second_value),
            )
        )
    ]
    for load in loads:
        load.start()

    barrier = pltpu.get_barrier_semaphore()
    for k in range(1, n):
        pl.semaphore_signal(barrier, inc=1, device_id={"fs": lax.rem(me + k, n)}, device_id_type=MESH)
    for k in range(1, tp):
        pl.semaphore_signal(barrier, inc=1, device_id={"tp": lax.rem(my_tp + k, tp)}, device_id_type=MESH)
    pl.semaphore_wait(barrier, n - 1 + tp - 1)

    lines = n // 4

    def gather(whole, own, send_sem, recv_sem, stacked):
        cols = own.shape[-1]
        cut = cols // 256 * 128
        spans = (pl.ds(0, cut), pl.ds(cut, cols - cut))
        rows = own.shape[0]

        def slot(owner, part):
            if stacked:
                return whole.at[owner, :, spans[part]]
            return whole.at[pl.ds(pl.multiple_of(owner * rows, rows), rows), spans[part]]

        return Gather(lines, slot, lambda part: own.at[:, spans[part]], send_sem, recv_sem)

    basis_g = gather(basis_all, basis, basis_send, basis_recv, False)
    master_g = gather(master_all, master, master_send, master_recv, False)
    dirs_g = gather(dirs_all, direction, dirs_send, dirs_recv, True)

    loads[0].wait()
    basis_g.along_z()
    steps, tail = basis_g.steps()
    steps[0]()
    loads[1].wait()
    loads[2].wait()
    cut = master_key_v.shape[1]
    master[:, :cut] = master_key_v[...].astype(BF16)
    master[:, cut:] = master_value_v[...].astype(BF16)
    early = lines
    master_g.along_z(1, early)
    rows = basis.shape[0]
    own_rows = pl.ds(pl.multiple_of(me * rows, rows), rows)
    basis_all[own_rows, :] = basis[...]
    master_all[own_rows, :] = master[...]
    for step in steps[1:]:
        step()
    master_steps, master_tail = master_g.steps()
    master_steps[0]()
    for step in tail:
        step()

    loads[3].wait()
    tokens = normed_v.shape[0]
    tile = 256

    @pl.loop(0, tokens // tile)
    def _(t):
        at = pl.ds(pl.multiple_of(t * tile, tile), tile)
        projected[at, :] = jnp.dot(normed_v[at, :], basis_all[...], preferred_element_type=F32).astype(BF16)

    loads[4].wait()
    loads[5].wait()
    kc = key_v.shape[1]
    rank_rows = first_key.shape[0]

    def project(cot, base):
        width = cot.shape[1]
        step = min(width, 512)
        for c in range(0, width, step):
            sums = lax.dot_general(
                projected[...], cot[:, c : c + step], (((0,), (0,)), ((), ())), preferred_element_type=F32
            ).astype(BF16)
            for j in range(n):
                partial[j, :, base + c : base + c + step] = sums[j * rank_rows : (j + 1) * rank_rows, :]

    project(key_v, 0)
    project(value_v, kc)

    part_copies = []
    for k in range(1, n):
        target = lax.rem(me + k, n)
        copy = pltpu.make_async_remote_copy(
            src_ref=partial.at[target],
            dst_ref=received.at[k],
            send_sem=part_send.at[k],
            recv_sem=part_recv.at[k],
            device_id={"fs": target},
            device_id_type=MESH,
        )
        copy.start()
        part_copies.append(copy)
    low = partial[me].astype(F32)
    received[0] = partial[me]
    master_g.along_z(early, lines)
    turns = [len(master_steps) * part // 16 for part in SHARES]
    for step in master_steps[1 : turns[0]]:
        step()
    for k, copy in enumerate(part_copies):
        copy.wait_recv()
    low = received[0].astype(F32)
    for k in range(1, n):
        low = low + received[k].astype(F32)

    square = jnp.sum(low * low)
    own_square[...] = jnp.full(own_square.shape, square, F32)
    squares[0] = jnp.full(own_square.shape, square, F32)
    square_copies = []
    for k in range(1, n):
        copy = pltpu.make_async_remote_copy(
            src_ref=own_square,
            dst_ref=squares.at[k],
            send_sem=square_send.at[k],
            recv_sem=square_recv.at[k],
            device_id={"fs": lax.rem(me + k, n)},
            device_id_type=MESH,
        )
        copy.start()
        square_copies.append(copy)
    for step in master_steps[turns[0] : turns[1]]:
        step()
    for copy in square_copies:
        copy.wait_recv()
    chip_square[...] = jnp.sum(squares[...], axis=0)
    chip_squares[0] = jnp.sum(squares[...], axis=0)
    chip_copies = []
    for k in range(1, tp):
        copy = pltpu.make_async_remote_copy(
            src_ref=chip_square,
            dst_ref=chip_squares.at[k],
            send_sem=chip_send.at[k],
            recv_sem=chip_recv.at[k],
            device_id={"tp": lax.rem(my_tp + k, tp)},
            device_id_type=MESH,
        )
        copy.start()
        chip_copies.append(copy)
    for copy in chip_copies:
        copy.wait_recv()
    total = jnp.sum(chip_squares[...], axis=0)[0:1, 0:1]
    grad_scale = 1.0 / jnp.sqrt(total / count + norm_eps)

    def update(scaled, first, second, base):
        moved = beta_first * first[...] + (1.0 - beta_first) * scaled
        spread = beta_second * second[...] + (1.0 - beta_second) * scaled * scaled
        turned = (moved / (jnp.sqrt(spread) + epsilon)).astype(BF16)
        direction[:, base : base + turned.shape[1]] = turned
        dirs_all[me, :, base : base + turned.shape[1]] = turned

    for load in loads[6:]:
        load.wait()
    scaled = low * grad_scale
    scaled_out[...] = scaled
    update(scaled[:, :kc], first_key, second_key, 0)
    update(scaled[:, kc:], first_value, second_value, kc)

    dirs_g.along_z()
    dirs_steps, dirs_tail = dirs_g.steps()
    dirs_steps[0]()
    for step in master_steps[turns[1] : turns[2]] + dirs_steps[1:] + master_steps[turns[2] :]:
        step()
    for step in dirs_tail + master_tail:
        step()
    for g in (basis_g, master_g, dirs_g):
        g.close()
    for copy in part_copies + square_copies + chip_copies:
        copy.wait_send()


def final_kernel(
    basis_all,
    master_all,
    dirs,
    basis,
    master_key,
    master_value,
    scaled,
    first_key,
    second_key,
    first_value,
    second_value,
    copy_key,
    copy_value,
    step_key,
    step_value,
    new_key,
    new_value,
    new_first_key,
    new_second_key,
    new_first_value,
    new_second_value,
):
    kc = copy_key.shape[1]
    for cut, out in ((slice(0, kc), copy_key), (slice(kc, None), copy_value)):
        step = jnp.dot(basis_all[...], dirs[:, cut], preferred_element_type=F32)
        out[...] = (master_all[:, cut].astype(F32) - learn_rate * step).astype(BF16)

    @pl.when(pl.program_id(0) == 0)
    def _():
        for cut, master, step_out, new in (
            (slice(0, kc), master_key, step_key, new_key),
            (slice(kc, None), master_value, step_value, new_value),
        ):
            step = jnp.dot(basis[...], dirs[:, cut], preferred_element_type=F32)
            step_out[...] = step
            new[...] = master[...] - learn_rate * step
        for cut, first, second, new_first, new_second in (
            (slice(0, kc), first_key, second_key, new_first_key, new_second_key),
            (slice(kc, None), first_value, second_value, new_first_value, new_second_value),
        ):
            own = scaled[:, cut]
            new_first[...] = beta_first * first[...] + (1.0 - beta_first) * own
            new_second[...] = beta_second * second[...] + (1.0 - beta_second) * own * own


def on_device(
    n,
    tp,
    normed,
    key_cot,
    value_cot,
    basis,
    master_key,
    master_value,
    first_key,
    second_key,
    first_value,
    second_value,
):
    rows, rank = basis.shape
    d = rows * n
    kc, vc = key_cot.shape[1], value_cot.shape[1]
    cols = kc + vc
    tokens = normed.shape[0]
    rank_rows = first_key.shape[0]
    lines = n // 4
    vmem = pl.BlockSpec(memory_space=pltpu.VMEM)
    hbm = pl.BlockSpec(memory_space=pl.ANY)
    dma = pltpu.SemaphoreType.DMA
    small = (8, 128)
    basis_all, master_all, dirs, scaled = pl.pallas_call(
        functools.partial(exchange_kernel, n, tp, rank * cols * tp),
        out_shape=(
            jax.ShapeDtypeStruct((d, rank), BF16),
            jax.ShapeDtypeStruct((d, cols), BF16),
            jax.ShapeDtypeStruct((n, rank_rows, cols), BF16),
            jax.ShapeDtypeStruct((rank_rows, cols), F32),
        ),
        in_specs=[hbm] * 10,
        out_specs=[vmem] * 4,
        scratch_shapes=[
            pltpu.VMEM(normed.shape, BF16),
            pltpu.VMEM(key_cot.shape, BF16),
            pltpu.VMEM(value_cot.shape, BF16),
            pltpu.VMEM(basis.shape, BF16),
            pltpu.VMEM(master_key.shape, F32),
            pltpu.VMEM(master_value.shape, F32),
            pltpu.VMEM(first_key.shape, F32),
            pltpu.VMEM(first_key.shape, F32),
            pltpu.VMEM(first_value.shape, F32),
            pltpu.VMEM(first_value.shape, F32),
            pltpu.VMEM((rows, cols), BF16),
            pltpu.VMEM((tokens, rank), BF16),
            pltpu.VMEM((n, rank_rows, cols), BF16),
            pltpu.VMEM((n, rank_rows, cols), BF16),
            pltpu.VMEM((rank_rows, cols), BF16),
            pltpu.VMEM(small, F32),
            pltpu.VMEM((n, *small), F32),
            pltpu.VMEM(small, F32),
            pltpu.VMEM((tp, *small), F32),
            dma((10,)),
        ]
        + [dma((2, 4 * lines))] * 6
        + [dma((n,))] * 4
        + [dma((tp,))] * 2,
        compiler_params=pltpu.CompilerParams(
            collective_id=0, has_side_effects=True, vmem_limit_bytes=67_043_328
        ),
    )(normed, key_cot, value_cot, basis, master_key, master_value, first_key, second_key, first_value, second_value)
    dirs = dirs.reshape(rank, cols)

    block = d // 2
    whole = lambda *shape: pl.BlockSpec(shape, lambda i: (0,) * len(shape))
    sliced = lambda width: pl.BlockSpec((block, width), lambda i: (i, 0))
    moments = [whole(rank_rows, kc)] * 2 + [whole(rank_rows, vc)] * 2
    copy_key, copy_value, step_key, step_value, new_key, new_value, nfk, nsk, nfv, nsv = pl.pallas_call(
        final_kernel,
        grid=(d // block,),
        out_shape=(
            jax.ShapeDtypeStruct((d, kc), BF16),
            jax.ShapeDtypeStruct((d, vc), BF16),
            jax.ShapeDtypeStruct((rows, kc), F32),
            jax.ShapeDtypeStruct((rows, vc), F32),
            jax.ShapeDtypeStruct((rows, kc), F32),
            jax.ShapeDtypeStruct((rows, vc), F32),
            jax.ShapeDtypeStruct(first_key.shape, F32),
            jax.ShapeDtypeStruct(first_key.shape, F32),
            jax.ShapeDtypeStruct(first_value.shape, F32),
            jax.ShapeDtypeStruct(first_value.shape, F32),
        ),
        in_specs=[
            sliced(rank),
            sliced(cols),
            whole(rank, cols),
            whole(rows, rank),
            whole(rows, kc),
            whole(rows, vc),
            whole(rank_rows, cols),
            *moments,
        ],
        out_specs=[sliced(kc), sliced(vc), whole(rows, kc), whole(rows, vc), whole(rows, kc), whole(rows, vc), *moments],
    )(
        basis_all, master_all, dirs, basis, master_key, master_value, scaled, first_key, second_key, first_value, second_value
    )
    return (step_key, step_value, new_key, new_value, copy_key, copy_value, nfk, nsk, nfv, nsv)


def solution(mesh):
    split = P("fs", "tp")
    lone = P("fs", None)
    return jax.shard_map(
        functools.partial(on_device, mesh.shape["fs"], mesh.shape["tp"]),
        mesh=mesh,
        in_specs=(lone, split, split, lone) + (split,) * 6,
        out_specs=(split,) * 4 + (P(None, "tp"),) * 2 + (split,) * 4,
        check_vma=False,
    )
```
